32 devices in a mesh: sp: 4 (over z), fs: 4 (over y, x), tp: 2 (over core).
Axes of the slice: x: 2, y: 2, z: 4, core: 2. Of those that a mesh axis runs over, the one named last changes fastest.
Arguments:
- tokens: bfloat16 [4, 2048, 2048], P('fs', ('sp', 'tp')), may hold values from -6 to 6
- input_gain: float32 [2048], replicated, may hold values from 0.1 to 1.9
- query_weight: bfloat16 [2048, 768], P(None, 'tp'), may hold values from -0.125 to 0.125
- latent_down: bfloat16 [2048, 256], replicated, may hold values from -0.125 to 0.125
- rotary_down: bfloat16 [2048, 32], replicated, may hold values from -0.125 to 0.125
- pool_down: bfloat16 [2048, 1024], P(None, 'tp'), may hold values from -0.125 to 0.125
- key_up: bfloat16 [256, 512], replicated, may hold values from -0.375 to 0.375
- value_up: bfloat16 [256, 1024], replicated, may hold values from -1.125 to 1.125, as said below
- query_gain: float32 [96], replicated, may hold values from 0.1 to 1.9
- key_gain: float32 [96], replicated, may hold values from 0.1 to 1.9
- pool_weight: bfloat16 [16, 64, 64], replicated, may hold values from -2.25 to 2.25, as said below
- pool_scale: float32 [1024], P('tp'), may hold values from 0.1 to 1.9
- attention_gain: float32 [1024], P('tp'), may hold values from 0.1 to 1.9
- pool_gain: float32 [1024], P('tp'), may hold values from 0.1 to 1.9
- attention_out: bfloat16 [1024, 2048], P('tp'), may hold values from -0.125 to 0.125
- pool_out: bfloat16 [1024, 2048], P('tp'), may hold values from -0.125 to 0.125
Outputs:
- mixed: bfloat16 [4, 2048, 2048], P('fs', ('sp', 'tp'))
The draws below stay inside these ranges and needn't reach their ends.
Inputs may be any that keep to these rules, and one draw needn't show every extreme that they name: `value_up`: entries of order 256 ** -0.5 or larger. `pool_weight`: entries of order 64 ** -0.5 or larger.
All inputs are finite; a program needn't handle non-finite values.
Results may differ from the reference program's by a relative error of at most 0.015.
Values may be sent and summed in bfloat16 or wider, within the bound.
A program may use at most 64 MiB of HBM per device.

```python
import math
import jax
import jax.numpy as jnp
from jax import lax

D = 2048
HEADS = 8
NOPE_DIM = 64
ROPE_DIM = 32
VALUE_DIM = 128
KV_LATENT = 256
GROUPS = 16
GROUP_DIM = 64
QK_DIM = 96
POOL_WIDTH = 1024
SEQS = 4
LENGTH = 2048
HEAD_BLOCKS = 2


def draw_value_up(key, part):
    columns = jnp.arange(HEADS * VALUE_DIM, dtype=jnp.int32) // VALUE_DIM
    level = columns.astype(jnp.float32) / (HEADS - 1)
    base = jnp.clip(jax.random.normal(key, (KV_LATENT, HEADS * VALUE_DIM), jnp.float32), -6.0, 6.0)
    factor = 3.0 ** level
    return (base * factor[None, :] * KV_LATENT ** (-0.5)).astype(jnp.bfloat16)


def draw_pool_weight(key, part):
    level = jnp.arange(GROUPS, dtype=jnp.int32).astype(jnp.float32) / (GROUPS - 1)
    base = jnp.clip(jax.random.normal(key, (GROUPS, GROUP_DIM, GROUP_DIM), jnp.float32), -6.0, 6.0)
    factor = 3.0 ** level
    return (base * factor[:, None, None] * GROUP_DIM ** (-0.5)).astype(jnp.bfloat16)


def steps_of(stream_key, shape, split, least, high):
    def one(position, blocks):
        draws = jax.random.uniform(jax.random.fold_in(jax.random.fold_in(stream_key, 6), position), (blocks,), jnp.float32, least / len(split), high / len(split))
        return jnp.repeat(jnp.exp(draws), shape[position] // blocks).reshape((-1,) + (1,) * (len(shape) - position - 1))

    factor_of = one(*split[0])
    for cut in split[1:]:
        factor_of = factor_of * one(*cut)
    return factor_of


def centred(key, extent, deviation, bound, pieces=(), kind=jnp.bfloat16):
    entries = deviation * jax.random.normal(key, extent, jnp.float32)
    if pieces:
        entries = entries * steps_of(key, extent, pieces, -0.22, 0.18)
    return jnp.clip(entries, -bound, bound).astype(kind)


def setup_inputs(seed: int = 0) -> dict:
    streams_of = jax.random.split(jax.random.key(seed), 17)
    tokens = centred(streams_of[0], (SEQS, LENGTH, D), 1.0, 6.0, ((0, 4), (1, 8)))
    input_gain = jnp.clip(1.0 + 0.18 * jax.random.normal(streams_of[1], (D,), jnp.float32), 0.1, 1.9)
    query_weight = centred(streams_of[2], (D, HEADS * QK_DIM), D ** -0.5, 0.125, ((1, 2),))
    latent_down = centred(streams_of[3], (D, KV_LATENT), D ** -0.5, 0.125)
    rotary_down = centred(streams_of[4], (D, ROPE_DIM), D ** -0.5, 0.125)
    pool_down = centred(streams_of[5], (D, POOL_WIDTH), D ** -0.5, 0.125, ((1, 2),))
    key_up = centred(streams_of[6], (KV_LATENT, HEADS * NOPE_DIM), KV_LATENT ** -0.5, 0.375)
    value_up = draw_value_up(jax.random.fold_in(streams_of[16], 71), 0)
    query_gain = jnp.clip(1.0 + 0.18 * jax.random.normal(streams_of[8], (QK_DIM,), jnp.float32), 0.1, 1.9)
    key_gain = jnp.clip(1.0 + 0.18 * jax.random.normal(streams_of[9], (QK_DIM,), jnp.float32), 0.1, 1.9)
    pool_weight = draw_pool_weight(jax.random.fold_in(streams_of[16], 71), 0)
    pool_scale = jnp.clip(1.0 + 0.18 * jax.random.normal(streams_of[11], (POOL_WIDTH,), jnp.float32), 0.1, 1.9)
    attention_gain = jnp.clip(1.0 + 0.18 * jax.random.normal(streams_of[12], (HEADS * VALUE_DIM,), jnp.float32), 0.1, 1.9)
    pool_gain = jnp.clip(1.0 + 0.18 * jax.random.normal(streams_of[13], (POOL_WIDTH,), jnp.float32), 0.1, 1.9)
    attention_out = centred(streams_of[14], (HEADS * VALUE_DIM, D), (HEADS * VALUE_DIM + POOL_WIDTH) ** -0.5, 0.125, ((0, 2),))
    pool_out = centred(streams_of[15], (POOL_WIDTH, D), (HEADS * VALUE_DIM + POOL_WIDTH) ** -0.5, 0.125, ((0, 2),))
    return {"tokens": tokens, "input_gain": input_gain, "query_weight": query_weight, "latent_down": latent_down, "rotary_down": rotary_down, "pool_down": pool_down, "key_up": key_up, "value_up": value_up, "query_gain": query_gain, "key_gain": key_gain, "pool_weight": pool_weight, "pool_scale": pool_scale, "attention_gain": attention_gain, "pool_gain": pool_gain, "attention_out": attention_out, "pool_out": pool_out}


EPS = 1e-06
THETA = 10000.0
rim_rows = 16

def rms_scale(values):
    return lax.rsqrt(lax.optimization_barrier(jnp.mean(values * values, axis=-1, keepdims=True)) + EPS)

def rotate(values, positions):
    half = values.shape[-1] // 2
    inv_freq = 1.0 / THETA ** (jnp.arange(half, dtype=jnp.float32) / half)
    angle = positions[:, None, None] * inv_freq
    cosine = jnp.cos(angle)
    sine = jnp.sin(angle)
    first = values[..., :half]
    second = values[..., half:]
    return jnp.concatenate([first * cosine - second * sine, second * cosine + first * sine], axis=-1)

def head_vectors(raw, gain, positions):
    normal = raw * rms_scale(raw) * gain
    turned = rotate(normal[..., NOPE_DIM:], positions)
    return jnp.concatenate([normal[..., :NOPE_DIM], turned], axis=-1).astype(jnp.bfloat16)

def expand_keys(latent_rows, first, key_up, value_up, key_gain):
    count = latent_rows.shape[0]
    heads = key_up.shape[1] // NOPE_DIM
    latent = latent_rows[:, :KV_LATENT].astype(jnp.float32)
    latent_normed = (latent * rms_scale(latent)).astype(jnp.bfloat16)
    plain = jnp.dot(latent_normed, key_up, preferred_element_type=jnp.float32).reshape(count, heads, NOPE_DIM)
    values = jnp.dot(latent_normed, value_up, preferred_element_type=jnp.float32).astype(jnp.bfloat16)
    shared = latent_rows[:, KV_LATENT:].astype(jnp.float32)
    shared = jnp.broadcast_to(shared[:, None, :], (count, heads, ROPE_DIM))
    positions = (first + jnp.arange(count, dtype=jnp.int32)).astype(jnp.float32)
    keys = head_vectors(jnp.concatenate([plain, shared], axis=-1), key_gain, positions)
    return (keys, values.reshape(count, heads, VALUE_DIM))

def pool_mix(pool_input, before, group_ids, positions):
    count = pool_input.shape[0]
    groups = group_ids.shape[0]
    current = pool_input.astype(jnp.float32).reshape(count, groups, GROUP_DIM)
    extended = jnp.concatenate([before, pool_input], axis=0).astype(jnp.float32)
    extended = extended.reshape(count + rim_rows, groups, GROUP_DIM)
    window = jnp.left_shift(2, group_ids % 4).astype(jnp.float32)
    total = current
    for back in range(1, rim_rows):
        taken = (window > back).astype(jnp.float32)
        total = total + extended[rim_rows - back:rim_rows - back + count] * taken[None, :, None]
    divisor = jnp.minimum(positions[:, None] + 1.0, window[None, :])
    return (total / divisor[:, :, None] - current).astype(jnp.bfloat16)

def one_sequence(tokens, input_gain, query_weight, latent_down, rotary_down, pool_down, key_up, value_up, query_gain, key_gain, pool_weight, pool_scale, attention_gain, pool_gain, attention_out, pool_out):
    count = tokens.shape[0]
    source = tokens.astype(jnp.float32)
    normed = (source * rms_scale(source) * input_gain).astype(jnp.bfloat16)
    latent_rows = jnp.concatenate([jnp.dot(normed, latent_down, preferred_element_type=jnp.float32), jnp.dot(normed, rotary_down, preferred_element_type=jnp.float32)], axis=1).astype(jnp.bfloat16)
    query_raw = jnp.dot(normed, query_weight, preferred_element_type=jnp.float32).reshape(count, HEADS, QK_DIM)
    pool_input = jnp.dot(normed, pool_down, preferred_element_type=jnp.float32).astype(jnp.bfloat16)
    positions_int = jnp.arange(count, dtype=jnp.int32)
    positions = positions_int.astype(jnp.float32)
    queries = lax.optimization_barrier(head_vectors(query_raw, query_gain, positions)).astype(jnp.float32)
    keys, values = expand_keys(latent_rows, 0, key_up, value_up, key_gain)
    keys = lax.optimization_barrier(keys).astype(jnp.float32)
    values = lax.optimization_barrier(values).astype(jnp.float32)
    factor = 1.0 / math.sqrt(QK_DIM)
    qblock = math.gcd(count, 512)

    def attend_block(index):
        begin = index * qblock
        query_block = lax.dynamic_slice_in_dim(queries, begin, qblock, 0)
        scores = jnp.einsum('qhd,khd->hqk', query_block, keys) * factor
        query_pos = begin + jnp.arange(qblock, dtype=jnp.int32)
        visible = positions_int[None, None, :] <= query_pos[None, :, None]
        weights = jnp.where(visible, jnp.exp(scores), 0.0)
        rounded = lax.optimization_barrier(weights.astype(jnp.bfloat16)).astype(jnp.float32)
        numer = jnp.einsum('hqk,khd->qhd', rounded, values)
        denom = lax.optimization_barrier(jnp.sum(weights, axis=-1))
        return numer / jnp.transpose(denom)[:, :, None]
    attended = lax.map(attend_block, jnp.arange(count // qblock, dtype=jnp.int32))
    attended = attended.reshape(count, HEADS * VALUE_DIM)
    before = jnp.zeros((rim_rows, POOL_WIDTH), jnp.bfloat16)
    pooled_mean = pool_mix(pool_input, before, jnp.arange(GROUPS, dtype=jnp.int32), positions)
    pooled = jnp.einsum('rgc,gcd->rgd', pooled_mean.astype(jnp.float32), pool_weight.astype(jnp.float32))
    pooled = pooled.reshape(count, POOL_WIDTH) * pool_scale
    attention_mixed = (attended * rms_scale(attended) * attention_gain).astype(jnp.bfloat16)
    pool_mixed = (pooled * rms_scale(pooled) * pool_gain).astype(jnp.bfloat16)
    head_cols = HEADS * VALUE_DIM // HEAD_BLOCKS
    pool_cols = POOL_WIDTH // HEAD_BLOCKS
    total = jnp.zeros((count, D), jnp.float32)
    for member in range(HEAD_BLOCKS):
        term = jnp.dot(attention_mixed[:, member * head_cols:(member + 1) * head_cols], attention_out[member * head_cols:(member + 1) * head_cols], preferred_element_type=jnp.float32)
        term = term + jnp.dot(pool_mixed[:, member * pool_cols:(member + 1) * pool_cols], pool_out[member * pool_cols:(member + 1) * pool_cols], preferred_element_type=jnp.float32)
        total = total + lax.optimization_barrier(term.astype(jnp.bfloat16)).astype(jnp.float32)
    return total.astype(jnp.bfloat16)

def reference(tokens, input_gain, query_weight, latent_down, rotary_down, pool_down, key_up, value_up, query_gain, key_gain, pool_weight, pool_scale, attention_gain, pool_gain, attention_out, pool_out):
    results = []
    for sequence in range(SEQS):
        results.append(one_sequence(tokens[sequence], input_gain, query_weight, latent_down, rotary_down, pool_down, key_up, value_up, query_gain, key_gain, pool_weight, pool_scale, attention_gain, pool_gain, attention_out, pool_out))
    return jnp.stack(results)
```

```python
import functools
import math

import jax
import jax.numpy as jnp
import numpy as np
from jax import lax
from jax.experimental import pallas as pl
from jax.experimental.pallas import tpu as pltpu
from jax.sharding import PartitionSpec as P

HEADS = 8
NOPE_DIM = 64
ROPE_DIM = 32
VALUE_DIM = 128
KV_LATENT = 256
GROUPS = 16
GROUP_DIM = 64
QK_DIM = 96
EPS = 1e-06
THETA = 10000.0
RIM = 16
HALF = ROPE_DIM // 2
MESH = pl.DeviceIdType.MESH
F32 = jnp.float32
BF16 = jnp.bfloat16


def dot(a, b):
    return jnp.dot(a, b, preferred_element_type=F32)


def column_of(row, width):
    return jnp.transpose(jnp.broadcast_to(row, (128, width)))[:, :1]


def kernel(
    sp, tp,
    tokens_h, input_gain_h, query_w_h, latent_w_h, rotary_w_h, pool_w_h, key_up_h, value_up_h,
    query_gain_h, key_gain_h, mix_w_h, scale_h, att_gain_h, pool_gain_h, att_out_h, pool_out_h,
    cos_h, sin_h,
    out_ref,
    x_all, input_gain, query_w, latent_w, rotary_w, pool_w, key_up, value_up,
    query_gain, key_gain, mix_w, scale, att_gain, pool_gain, att_out, pool_out, cos_t, sin_t,
    normed, key_up_t, lat_buf, rot_buf, queries, keys_t, vals, acc, ext, rim_out, rim_in, blockdiag,
    pooled_ref, acc_pool, ss_buf, mixed, send_buf, recv_buf,
    load_sem, tok_send, tok_recv, z_send, z_recv, f_send, f_recv, rim_send, rim_recv,
    ss_send, ss_recv, out_send, out_recv,
):
    s = lax.axis_index("sp")
    m = lax.axis_index("tp")
    rows, width = tokens_h.shape
    block = rows * tp
    heads = HEADS // tp
    groups = GROUPS // tp
    chans = groups * GROUP_DIM
    chunks, _, _, cw = send_buf.shape

    def peer(j):
        return lax.rem(m + j, tp)

    def load(i, src, dst):
        return pltpu.make_async_copy(src, dst, load_sem.at[i])

    loads = {
        "x": load(0, tokens_h, x_all.at[m]),
        "ig": load(1, input_gain_h, input_gain),
        "lw": load(2, latent_w_h, latent_w),
        "rw": load(3, rotary_w_h, rotary_w),
        "pw": load(4, pool_w_h, pool_w),
        "qw": load(5, query_w_h, query_w),
        "qg": load(6, query_gain_h, query_gain),
        "kg": load(7, key_gain_h, key_gain),
        "cos": load(8, cos_h, cos_t),
        "sin": load(9, sin_h, sin_t),
        "ku": load(10, key_up_h, key_up),
        "vu": load(11, value_up_h.at[:, pl.ds(pl.multiple_of(m * heads * VALUE_DIM, 128), heads * VALUE_DIM)], value_up),
        "mw": load(12, mix_w_h.at[pl.ds(m * groups, groups)], mix_w),
        "sc": load(13, scale_h, scale),
        "pg": load(14, pool_gain_h, pool_gain),
        "po": load(15, pool_out_h, pool_out),
        "ag": load(16, att_gain_h, att_gain),
        "ao": load(17, att_out_h, att_out),
    }
    for item in loads.values():
        item.start()

    barrier = pltpu.get_barrier_semaphore()
    for j in range(1, tp):
        pl.semaphore_signal(barrier, inc=1, device_id={"tp": peer(j)}, device_id_type=MESH)
    for d in range(1, sp):
        pl.semaphore_signal(barrier, inc=1, device_id={"sp": lax.rem(s + d, sp)}, device_id_type=MESH)
    pl.semaphore_wait(barrier, tp - 1 + sp - 1)

    def remote(src, dst, ssem, rsem, where):
        return pltpu.make_async_remote_copy(
            src_ref=src, dst_ref=dst, send_sem=ssem, recv_sem=rsem, device_id=where, device_id_type=MESH
        )

    def tok_copy(j, owner):
        return remote(tokens_h, x_all.at[owner], tok_send.at[j], tok_recv.at[owner], {"tp": peer(j)})

    def z_copy(d, src):
        where = {"sp": lax.rem(s + d, sp)}
        return [
            remote(buf.at[src, m], buf.at[src, m], z_send.at[d, k], z_recv.at[src, k], where)
            for k, buf in enumerate((lat_buf, rot_buf))
        ]

    def f_copy(src, j, owner):
        where = {"tp": peer(j)}
        return [
            remote(buf.at[src, owner], buf.at[src, owner], f_send.at[src, j, k], f_recv.at[src, owner, k], where)
            for k, buf in enumerate((lat_buf, rot_buf))
        ]

    def rim_copy():
        return remote(rim_out, rim_in, rim_send.at[0], rim_recv.at[0], {"sp": lax.rem(s + 1, sp)})

    def ss_copy(k, j, owner):
        return remote(ss_buf.at[k, owner], ss_buf.at[k, owner], ss_send.at[k, j], ss_recv.at[k, owner], {"tp": peer(j)})

    def out_copy(c, j, owner):
        return remote(send_buf.at[c, peer(j)], recv_buf.at[c, owner], out_send.at[c, j], out_recv.at[c, owner], {"tp": peer(j)})

    for j in range(1, tp):
        tok_copy(j, m).start()

    step = min(64, rows)

    def norm_piece(piece):
        def body(i, carry):
            at = pl.multiple_of(i * step, step)
            x = x_all[piece, pl.ds(at, step), :].astype(F32)
            r = lax.rsqrt(jnp.mean(x * x, axis=-1, keepdims=True) + EPS)
            normed[piece, pl.ds(at, step), :] = (x * r * input_gain[...]).astype(BF16)
            return carry

        lax.fori_loop(0, rows // step, body, 0)

    loads["x"].wait()
    loads["ig"].wait()
    norm_piece(m)
    loads["lw"].wait()
    loads["rw"].wait()
    own = normed[m]
    lat_buf[s, m] = dot(own, latent_w[...]).astype(BF16)
    rot = dot(own, rotary_w[...])
    rot = jnp.concatenate([rot, jnp.zeros((rows, 128 - ROPE_DIM), F32)], axis=1)
    rot_buf[s, m] = jnp.transpose(rot)[:ROPE_DIM].astype(BF16)
    for d in range(1, sp):
        @pl.when(s + d < sp)
        def _():
            for c in z_copy(d, s):
                c.start()
    for j in range(1, tp):
        for c in f_copy(s, j, m):
            c.start()

    for j in range(1, tp):
        tok_copy(j, peer(j)).wait_recv()
        norm_piece(peer(j))

    full = normed[...].reshape(block, width)
    loads["pw"].wait()
    pool_in = dot(full, pool_w[...]).astype(BF16)
    ext[RIM:, :] = pool_in.astype(F32)
    rim_out[...] = pool_in[block - RIM :, :]

    @pl.when(s + 1 < sp)
    def _():
        rim_copy().start()

    loads["qw"].wait()
    loads["qg"].wait()
    loads["cos"].wait()
    loads["sin"].wait()
    query_t = jnp.transpose(dot(full, query_w[...]))
    factor = math.log2(math.e) / math.sqrt(QK_DIM)
    gain_q = column_of(query_gain[...], QK_DIM) * factor
    at = pl.multiple_of(s * block, 128)
    cosine = cos_t[:, pl.ds(at, block)]
    sine = sin_t[:, pl.ds(at, block)]
    pad = jnp.zeros((128 - QK_DIM, block), F32)
    for h in range(heads):
        u = query_t[h * QK_DIM : (h + 1) * QK_DIM]
        r = lax.rsqrt(jnp.sum(u * u, axis=0, keepdims=True) * (1.0 / QK_DIM) + EPS)
        n = u * r * gain_q
        a = n[NOPE_DIM : NOPE_DIM + HALF]
        b = n[NOPE_DIM + HALF :]
        turned = jnp.concatenate(
            [n[:NOPE_DIM], a * cosine - b * sine, b * cosine + a * sine, pad], axis=0
        )
        queries[h] = jnp.transpose(turned).astype(BF16)

    loads["ku"].wait()
    key_up_t[...] = jnp.transpose(key_up[...].astype(F32)).astype(BF16)
    loads["kg"].wait()
    gain_k = column_of(key_gain[...], QK_DIM)
    gain_k_plain = gain_k[:NOPE_DIM]
    gain_k_rot = gain_k[NOPE_DIM:]
    loads["vu"].wait()
    for h in range(heads):
        keys_t[h, QK_DIM:, :] = jnp.zeros((128 - QK_DIM, block), BF16)
        vals[h, :, VALUE_DIM:] = jnp.ones((block, VALUE_DIM), BF16)

    def expand(src):
        latent = lat_buf[src].reshape(block, KV_LATENT).astype(F32)
        r = lax.rsqrt(jnp.mean(latent * latent, axis=-1, keepdims=True) + EPS)
        latent_normed = (latent * r).astype(BF16)
        own_up = key_up_t[pl.ds(pl.multiple_of(m * heads * NOPE_DIM, 64), heads * NOPE_DIM), :]
        plain = lax.dot_general(
            own_up, latent_normed, (((1,), (1,)), ((), ())), preferred_element_type=F32
        )
        value = dot(latent_normed, value_up[...]).astype(BF16)
        pieces = [rot_buf[src, j].astype(F32) for j in range(tp)]
        shared = jnp.concatenate(pieces, axis=1) if tp > 1 else pieces[0]
        shared_sum = jnp.sum(shared * shared, axis=0, keepdims=True)
        first = pl.multiple_of(src * block, 128)
        cosine = cos_t[:, pl.ds(first, block)]
        sine = sin_t[:, pl.ds(first, block)]
        scaled = shared * gain_k_rot
        a = scaled[:HALF]
        b = scaled[HALF:]
        turned_a = a * cosine - b * sine
        turned_b = b * cosine + a * sine
        for h in range(heads):
            u = plain[h * NOPE_DIM : (h + 1) * NOPE_DIM]
            total = jnp.sum(u * u, axis=0, keepdims=True) + shared_sum
            r = lax.rsqrt(total * (1.0 / QK_DIM) + EPS)
            keys_t[h, :NOPE_DIM, :] = (u * gain_k_plain * r).astype(BF16)
            keys_t[h, NOPE_DIM : NOPE_DIM + HALF, :] = (turned_a * r).astype(BF16)
            keys_t[h, NOPE_DIM + HALF : QK_DIM, :] = (turned_b * r).astype(BF16)
            vals[h, :, :VALUE_DIM] = value[:, h * VALUE_DIM : (h + 1) * VALUE_DIM]

    qc = min(256, block)

    def attend(head, diagonal):
        for q0 in range(0, block, qc):
            span = q0 + qc if diagonal else block
            score = dot(queries[head, q0 : q0 + qc, :], keys_t[head, :, :span])
            weight = jnp.exp2(score)
            if diagonal:
                qpos = q0 + lax.broadcasted_iota(jnp.int32, (qc, span), 0)
                kpos = lax.broadcasted_iota(jnp.int32, (qc, span), 1)
                weight = jnp.where(kpos <= qpos, weight, 0.0)
            got = dot(weight.astype(BF16), vals[head, :span, :])
            if diagonal:
                acc[head, q0 : q0 + qc, :] = got
            else:
                acc[head, q0 : q0 + qc, :] += got

    for name in ("mw", "sc", "pg"):
        loads[name].wait()
    blockdiag[...] = jnp.zeros((chans, chans), BF16)
    for g in range(groups):
        lo = g * GROUP_DIM
        blockdiag[lo : lo + GROUP_DIM, lo : lo + GROUP_DIM] = mix_w[g]

    @pl.when(s > 0)
    def _():
        rim_copy().wait_recv()
        ext[:RIM, :] = rim_in[...].astype(F32)

    @pl.when(s == 0)
    def _():
        ext[:RIM, :] = jnp.zeros((RIM, chans), F32)

    def share_squares(k, total):
        line = jnp.transpose(jnp.broadcast_to(total, (block, 128)))[:8]
        ss_buf[k, m] = line
        for j in range(1, tp):
            ss_copy(k, j, m).start()

    def row_factor(k, count):
        for j in range(1, tp):
            ss_copy(k, j, peer(j)).wait_recv()
        total = ss_buf[k, 0]
        for j in range(1, tp):
            total = total + ss_buf[k, j]
        line = lax.rsqrt(total[:1] * (1.0 / count) + EPS)
        return jnp.transpose(jnp.broadcast_to(line, (128, block)))[:, :1]

    position = s * block + lax.broadcasted_iota(jnp.int32, (block, 1), 0)
    since = position.astype(F32) + 1.0
    square_total = jnp.zeros((block, 1), F32)
    pw = 128
    means = []
    for c0 in range(0, chans, pw):
        current = ext[:, c0 : c0 + pw]
        channel = c0 + lax.broadcasted_iota(jnp.int32, (1, pw), 1)
        group = m * groups + channel // GROUP_DIM
        kind = lax.rem(group, 4)
        total = current
        chosen = jnp.zeros((block, pw), F32)
        for level in range(4):
            total = total + pltpu.roll(total, 1 << level, 0)
            share = 1.0 / jnp.minimum(since, float(2 << level))
            chosen = jnp.where(kind == level, total[RIM:] * share, chosen)
        means.append((chosen - current[RIM:]).astype(BF16))
    pooled = dot(jnp.concatenate(means, axis=1) if len(means) > 1 else means[0], blockdiag[...])
    pooled = pooled * scale[...]
    pooled_ref[...] = pooled
    share_squares(0, jnp.sum(pooled * pooled, axis=1, keepdims=True))

    for j in range(1, tp):
        for c in f_copy(s, j, peer(j)):
            c.wait_recv()
    expand(s)
    for h in range(heads):
        attend(h, True)

    pool_factor = row_factor(0, GROUPS * GROUP_DIM)
    mixed[...] = (pooled_ref[...] * pool_factor * pool_gain[...]).astype(BF16)
    loads["po"].wait()
    pool_mixed = mixed[...]

    def pool_chunk(c, carry):
        at = pl.multiple_of(c * cw, 128)
        acc_pool[:, pl.ds(at, cw)] = dot(pool_mixed, pool_out[:, pl.ds(at, cw)])
        return carry

    lax.fori_loop(0, chunks, pool_chunk, 0)

    def earlier(d, carry):
        src = s - d
        for c in z_copy(0, src):
            c.wait_recv()
        for j in range(1, tp):
            for c in f_copy(src, j, m):
                c.start()
        for j in range(1, tp):
            for c in f_copy(src, j, peer(j)):
                c.wait_recv()
        expand(src)
        for h in range(heads):
            attend(h, False)
        return carry

    lax.fori_loop(1, s + 1, earlier, 0)

    loads["ag"].wait()
    square_total = jnp.zeros((block, 1), F32)
    for h in range(heads):
        lo = h * VALUE_DIM
        one = acc[h, :, :VALUE_DIM] / acc[h, :, VALUE_DIM:]
        square_total = square_total + jnp.sum(one * one, axis=1, keepdims=True)
        mixed[:, lo : lo + VALUE_DIM] = (one * att_gain[:, lo : lo + VALUE_DIM]).astype(BF16)
    share_squares(1, square_total)
    loads["ao"].wait()
    factor_att = row_factor(1, HEADS * VALUE_DIM)
    att_mixed = mixed[...]
    for c in range(chunks):
        lo = c * cw
        part = dot(att_mixed, att_out[:, lo : lo + cw]) * factor_att + acc_pool[:, lo : lo + cw]
        send_buf[c] = part.astype(BF16).reshape(tp, rows, cw)
        for j in range(1, tp):
            out_copy(c, j, m).start()
    for c in range(chunks):
        total = send_buf[c, m].astype(F32)
        for j in range(1, tp):
            out_copy(c, j, peer(j)).wait_recv()
            total = total + recv_buf[c, peer(j)].astype(F32)
        out_ref[:, c * cw : (c + 1) * cw] = total.astype(BF16)

    for j in range(1, tp):
        tok_copy(j, m).wait_send()
        for k in range(2):
            ss_copy(k, j, m).wait_send()
        for c in range(chunks):
            out_copy(c, j, m).wait_send()
    for d in range(1, sp):
        @pl.when(s + d < sp)
        def _():
            for c in z_copy(d, s):
                c.wait_send()

    @pl.when(s + 1 < sp)
    def _():
        rim_copy().wait_send()

    def drain(src, carry):
        for j in range(1, tp):
            for c in f_copy(src, j, m):
                c.wait_send()
        return carry

    lax.fori_loop(0, s + 1, drain, 0)


def turn_tables(length):
    steps = np.arange(HALF, dtype=np.float32) / np.float32(HALF)
    inv_freq = np.float32(1.0) / np.power(np.float32(THETA), steps).astype(np.float32)
    angle = inv_freq[:, None] * np.arange(length, dtype=np.float32)[None, :]
    angle = angle.astype(np.float32).astype(np.float64)
    return np.cos(angle).astype(np.float32), np.sin(angle).astype(np.float32)


def local(
    tokens, input_gain, query_weight, latent_down, rotary_down, pool_down, key_up, value_up,
    query_gain, key_gain, pool_weight, pool_scale, attention_gain, pool_gain, attention_out, pool_out,
):
    sp = lax.axis_size("sp")
    tp = lax.axis_size("tp")
    _, rows, width = tokens.shape
    block = rows * tp
    heads = HEADS // tp
    groups = GROUPS // tp
    chans = groups * GROUP_DIM
    cosine, sine = turn_tables(block * sp)
    chunks = 4
    cw = width // chunks
    line = lambda v: v.reshape(1, -1)
    operands = [
        tokens[0], line(input_gain), query_weight, latent_down, rotary_down, pool_down, key_up, value_up,
        line(query_gain), line(key_gain), pool_weight, line(pool_scale), line(attention_gain),
        line(pool_gain), attention_out, pool_out, jnp.asarray(cosine), jnp.asarray(sine),
    ]
    V = pltpu.VMEM
    D = pltpu.SemaphoreType.DMA
    held = [V(o.shape, o.dtype) for o in operands]
    held[0] = V((tp, rows, width), BF16)
    held[7] = V((KV_LATENT, heads * VALUE_DIM), BF16)
    held[10] = V((groups, GROUP_DIM, GROUP_DIM), BF16)
    scratch = held + [
        V((tp, rows, width), BF16),
        V((HEADS * NOPE_DIM, KV_LATENT), BF16),
        V((sp, tp, rows, KV_LATENT), BF16),
        V((sp, tp, ROPE_DIM, rows), BF16),
        V((heads, block, 128), BF16),
        V((heads, 128, block), BF16),
        V((heads, block, 2 * VALUE_DIM), BF16),
        V((heads, block, 2 * VALUE_DIM), F32),
        V((block + RIM, chans), F32),
        V((RIM, chans), BF16),
        V((RIM, chans), BF16),
        V((chans, chans), BF16),
        V((block, chans), F32),
        V((block, width), F32),
        V((2, tp, 8, block), F32),
        V((block, chans), BF16),
        V((chunks, tp, rows, cw), BF16),
        V((chunks, tp, rows, cw), BF16),
        D((len(operands),)),
        D((tp,)), D((tp,)),
        D((sp, 2)), D((sp, 2)),
        D((sp, tp, 2)), D((sp, tp, 2)),
        D((1,)), D((1,)),
        D((2, tp)), D((2, tp)),
        D((chunks, tp)), D((chunks, tp)),
    ]
    out = pl.pallas_call(
        functools.partial(kernel, sp, tp),
        out_shape=jax.ShapeDtypeStruct((rows, width), BF16),
        in_specs=[pl.BlockSpec(memory_space=pl.ANY)] * len(operands),
        out_specs=pl.BlockSpec(memory_space=pltpu.VMEM),
        scratch_shapes=scratch,
        compiler_params=pltpu.CompilerParams(
            collective_id=0, has_side_effects=True, vmem_limit_bytes=58 * 1024 * 1024
        ),
    )(*operands)
    return out[None]


def solution(mesh):
    placed = (
        P("fs", ("sp", "tp"), None), P(), P(None, "tp"), P(), P(), P(None, "tp"), P(), P(),
        P(), P(), P(), P("tp"), P("tp"), P("tp"), P("tp", None), P("tp", None),
    )
    return jax.shard_map(
        local, mesh=mesh, in_specs=placed, out_specs=P("fs", ("sp", "tp"), None), check_vma=False
    )
```

```python
import functools
import math

import jax
import jax.numpy as jnp
import numpy as np
from jax import lax
from jax.experimental import pallas as pl
from jax.experimental.pallas import tpu as pltpu
from jax.sharding import PartitionSpec as P

HEADS = 8
NOPE_DIM = 64
ROPE_DIM = 32
VALUE_DIM = 128
KV_LATENT = 256
GROUPS = 16
GROUP_DIM = 64
QK_DIM = 96
EPS = 1e-06
THETA = 10000.0
RIM = 16
HALF = ROPE_DIM // 2
MESH = pl.DeviceIdType.MESH
F32 = jnp.float32
BF16 = jnp.bfloat16


def dot(a, b):
    return jnp.dot(a, b, preferred_element_type=F32)


def column_of(row, width):
    return jnp.transpose(jnp.broadcast_to(row, (128, width)))[:, :1]


def kernel(
    sp, tp,
    tokens_h, input_gain_h, query_w_h, latent_w_h, rotary_w_h, pool_w_h, key_up_h, value_up_h,
    query_gain_h, key_gain_h, mix_w_h, scale_h, att_gain_h, pool_gain_h, att_out_h, pool_out_h,
    cos_h, sin_h,
    out_ref,
    x_all, input_gain, query_w, latent_w, rotary_w, pool_w, key_up, value_up,
    query_gain, key_gain, mix_w, scale, att_gain, pool_gain, att_out, pool_out, cos_t, sin_t,
    normed, key_up_t, lat_buf, rot_buf, queries, keys_t, vals, acc, ext, tail_in, blockdiag,
    pooled_ref, acc_pool, ss_buf, mixed, send_buf, recv_buf,
    load_sem, tok_send, tok_recv, z_send, z_recv, f_send, f_recv, tail_send, tail_recv,
    ss_send, ss_recv, out_send, out_recv,
):
    s = lax.axis_index("sp")
    m = lax.axis_index("tp")
    rows, width = tokens_h.shape
    block = rows * tp
    heads = HEADS // tp
    groups = GROUPS // tp
    chans = groups * GROUP_DIM
    chunks, _, _, cw = send_buf.shape

    def peer(j):
        return lax.rem(m + j, tp)

    def load(i, src, dst):
        return pltpu.make_async_copy(src, dst, load_sem.at[i])

    loads = {
        "x": load(0, tokens_h, x_all.at[m]),
        "ig": load(1, input_gain_h, input_gain),
        "lw": load(2, latent_w_h, latent_w),
        "rw": load(3, rotary_w_h, rotary_w),
        "pw": load(4, pool_w_h, pool_w),
        "qw": load(5, query_w_h, query_w),
        "qg": load(6, query_gain_h, query_gain),
        "kg": load(7, key_gain_h, key_gain),
        "cos": load(8, cos_h, cos_t),
        "sin": load(9, sin_h, sin_t),
        "ku": load(10, key_up_h, key_up),
        "vu": load(11, value_up_h.at[:, pl.ds(pl.multiple_of(m * heads * VALUE_DIM, 128), heads * VALUE_DIM)], value_up),
        "mw": load(12, mix_w_h.at[pl.ds(m * groups, groups)], mix_w),
        "sc": load(13, scale_h, scale),
        "pg": load(14, pool_gain_h, pool_gain),
        "po": load(15, pool_out_h, pool_out),
        "ag": load(16, att_gain_h, att_gain),
        "ao": load(17, att_out_h, att_out),
    }
    for item in loads.values():
        item.start()

    barrier = pltpu.get_barrier_semaphore()
    for j in range(1, tp):
        pl.semaphore_signal(barrier, inc=1, device_id={"tp": peer(j)}, device_id_type=MESH)
    for d in range(1, sp):
        @pl.when(s >= d)
        def _():
            pl.semaphore_signal(barrier, inc=1, device_id={"sp": lax.rem(s + sp - d, sp)}, device_id_type=MESH)

    @pl.when(jnp.logical_and(s > 0, m < tp - 1))
    def _():
        where = {"sp": lax.rem(s + sp - 1, sp), "tp": tp - 1}
        pl.semaphore_signal(barrier, inc=1, device_id=where, device_id_type=MESH)

    def remote(src, dst, ssem, rsem, where):
        return pltpu.make_async_remote_copy(
            src_ref=src, dst_ref=dst, send_sem=ssem, recv_sem=rsem, device_id=where, device_id_type=MESH
        )

    def tok_copy(j, owner):
        return remote(tokens_h, x_all.at[owner], tok_send.at[j], tok_recv.at[owner], {"tp": peer(j)})

    def z_copy(hop, src):
        where = {"sp": lax.rem(s + hop + 1, sp)}
        return [
            remote(buf.at[src, m], buf.at[src, m], z_send.at[src, hop, k], z_recv.at[src, k], where)
            for k, buf in enumerate((lat_buf, rot_buf))
        ]

    odd = lax.rem(s, 2)
    hops = ((0, s + 1 < sp), (1, jnp.logical_and(s + 2 < sp, odd == 0)))

    def relays(d):
        return jnp.logical_and(s + 1 < sp, jnp.logical_or(odd == 0, d > 1))

    def arrive(d):
        src = s - d
        for c in z_copy(0, src):
            c.wait_recv()

        @pl.when(relays(d))
        def _():
            for c in z_copy(0, src):
                c.start()

        for j in range(1, tp):
            for c in f_copy(src, j, m):
                c.start()

    def f_copy(src, j, owner):
        where = {"tp": peer(j)}
        return [
            remote(buf.at[src, owner], buf.at[src, owner], f_send.at[src, j, k], f_recv.at[src, owner, k], where)
            for k, buf in enumerate((lat_buf, rot_buf))
        ]

    def tail_copy(j):
        where = {"sp": lax.rem(s + 1, sp), "tp": j}
        return remote(tokens_h.at[rows - RIM :, :], tail_in, tail_send.at[j], tail_recv.at[0], where)

    def ss_copy(k, j, owner):
        return remote(ss_buf.at[k, owner], ss_buf.at[k, owner], ss_send.at[k, j], ss_recv.at[k, owner], {"tp": peer(j)})

    def out_copy(c, j, owner):
        return remote(send_buf.at[c, peer(j)], recv_buf.at[c, owner], out_send.at[c, j], out_recv.at[c, owner], {"tp": peer(j)})

    apart = rows % 128 == 0
    step = min(64, rows)

    def slot_of(piece):
        return lax.rem(piece - m + tp, tp) if apart else piece

    def norm_rows(x):
        x = x.astype(F32)
        r = lax.rsqrt(jnp.mean(x * x, axis=-1, keepdims=True) + EPS)
        return (x * r * input_gain[...]).astype(BF16)

    def norm_piece(piece):
        first = slot_of(piece) * rows

        def body(i, carry):
            at = pl.multiple_of(i * step, step)
            to = pl.multiple_of(first + i * step, step)
            normed[pl.ds(to, step), :] = norm_rows(x_all[piece, pl.ds(at, step), :])
            return carry

        lax.fori_loop(0, rows // step, body, 0)

    loads["x"].wait()
    loads["ig"].wait()
    norm_piece(m)

    later = sp - 1 - s
    sends_tail = lax.div(m + 1, tp) * lax.div(later + max(sp - 2, 0), max(sp - 1, 1))
    pl.semaphore_wait(barrier, tp - 1 + later + sends_tail * (tp - 1))

    for j in range(1, tp):
        tok_copy(j, m).start()

    @pl.when(jnp.logical_and(s + 1 < sp, m == tp - 1))
    def _():
        for j in range(tp):
            tail_copy(j).start()

    loads["lw"].wait()
    loads["rw"].wait()
    own = normed[pl.ds(pl.multiple_of(slot_of(m) * rows, rows), rows), :]
    rot_buf[s, m] = lax.dot_general(
        rotary_w[...], own, (((1,), (1,)), ((), ())), preferred_element_type=F32
    ).astype(BF16)
    lat_buf[s, m] = dot(own, latent_w[...]).astype(BF16)
    for hop, wanted in hops:
        @pl.when(wanted)
        def _():
            for c in z_copy(hop, s):
                c.start()
    for j in range(1, tp):
        for c in f_copy(s, j, m):
            c.start()

    loads["qw"].wait()
    loads["qg"].wait()
    loads["cos"].wait()
    loads["sin"].wait()
    factor = math.log2(math.e) / math.sqrt(QK_DIM)
    gain_q = column_of(query_gain[...], QK_DIM) * factor

    def project(slot, at, count, last):
        offset = slot * rows
        query_t = jnp.transpose(dot(normed[offset : offset + count, :], query_w[...]))
        first = pl.multiple_of(s * block + at, 128)
        cosine = cos_t[:, pl.ds(first, count)]
        sine = sin_t[:, pl.ds(first, count)]
        pad = jnp.zeros((128 - QK_DIM, count), F32)
        for h in range(heads):
            u = query_t[h * QK_DIM : (h + 1) * QK_DIM]
            r = lax.rsqrt(jnp.sum(u * u, axis=0, keepdims=True) * (1.0 / QK_DIM) + EPS)
            n = u * r * gain_q
            a = n[NOPE_DIM : NOPE_DIM + HALF]
            b = n[NOPE_DIM + HALF :]
            turned = jnp.concatenate(
                [n[:NOPE_DIM], a * cosine - b * sine, b * cosine + a * sine, pad], axis=0
            )
            queries[h, pl.ds(at, count), :] = jnp.transpose(turned).astype(BF16)
        taken = count
        if last:
            @pl.when(s > 0)
            def _():
                tail_copy(0).wait_recv()
                normed[block:, :] = norm_rows(tail_in[...])

            @pl.when(s == 0)
            def _():
                normed[block:, :] = jnp.zeros((RIM, width), BF16)

            taken = count + RIM
        pool_in = dot(normed[offset : offset + taken, :], pool_w[...]).astype(BF16).astype(F32)
        ext[pl.ds(pl.multiple_of(RIM + at, RIM), count), :] = pool_in[:count]
        if last:
            ext[:RIM, :] = pool_in[count:]

    loads["pw"].wait()
    if apart:
        for j in range(tp):
            if j > 0:
                tok_copy(j, peer(j)).wait_recv()
                norm_piece(peer(j))
            project(j, pl.multiple_of(peer(j) * rows, rows), rows, j == tp - 1)
    else:
        for j in range(1, tp):
            tok_copy(j, peer(j)).wait_recv()
            norm_piece(peer(j))
        project(0, 0, block, True)

    loads["ku"].wait()
    key_up_t[...] = jnp.transpose(key_up[...].astype(F32)).astype(BF16)
    loads["kg"].wait()
    gain_k = column_of(key_gain[...], QK_DIM)
    gain_k_plain = gain_k[:NOPE_DIM]
    gain_k_rot = gain_k[NOPE_DIM:]
    loads["vu"].wait()
    for h in range(heads):
        keys_t[h, QK_DIM:, :] = jnp.zeros((128 - QK_DIM, block), BF16)
        vals[h, :, VALUE_DIM:] = jnp.ones((block, VALUE_DIM), BF16)

    def expand(src):
        latent = lat_buf[src].reshape(block, KV_LATENT).astype(F32)
        r = lax.rsqrt(jnp.mean(latent * latent, axis=-1, keepdims=True) + EPS)
        latent_normed = (latent * r).astype(BF16)
        own_up = key_up_t[pl.ds(pl.multiple_of(m * heads * NOPE_DIM, 64), heads * NOPE_DIM), :]
        plain = lax.dot_general(
            own_up, latent_normed, (((1,), (1,)), ((), ())), preferred_element_type=F32
        )
        value = dot(latent_normed, value_up[...]).astype(BF16)
        pieces = [rot_buf[src, j].astype(F32) for j in range(tp)]
        shared = jnp.concatenate(pieces, axis=1) if tp > 1 else pieces[0]
        shared_sum = jnp.sum(shared * shared, axis=0, keepdims=True)
        first = pl.multiple_of(src * block, 128)
        cosine = cos_t[:, pl.ds(first, block)]
        sine = sin_t[:, pl.ds(first, block)]
        scaled = shared * gain_k_rot
        a = scaled[:HALF]
        b = scaled[HALF:]
        turned_a = a * cosine - b * sine
        turned_b = b * cosine + a * sine
        for h in range(heads):
            u = plain[h * NOPE_DIM : (h + 1) * NOPE_DIM]
            total = jnp.sum(u * u, axis=0, keepdims=True) + shared_sum
            r = lax.rsqrt(total * (1.0 / QK_DIM) + EPS)
            keys_t[h, :NOPE_DIM, :] = (u * gain_k_plain * r).astype(BF16)
            keys_t[h, NOPE_DIM : NOPE_DIM + HALF, :] = (turned_a * r).astype(BF16)
            keys_t[h, NOPE_DIM + HALF : QK_DIM, :] = (turned_b * r).astype(BF16)
            vals[h, :, :VALUE_DIM] = value[:, h * VALUE_DIM : (h + 1) * VALUE_DIM]

    qc = min(256, block)

    def attend(head, diagonal):
        for q0 in range(0, block, qc):
            span = q0 + qc if diagonal else block
            score = dot(queries[head, q0 : q0 + qc, :], keys_t[head, :, :span])
            weight = jnp.exp2(score)
            if diagonal:
                qpos = q0 + lax.broadcasted_iota(jnp.int32, (qc, span), 0)
                kpos = lax.broadcasted_iota(jnp.int32, (qc, span), 1)
                weight = jnp.where(kpos <= qpos, weight, 0.0)
            got = dot(weight.astype(BF16), vals[head, :span, :])
            if diagonal:
                acc[head, q0 : q0 + qc, :] = got
            else:
                acc[head, q0 : q0 + qc, :] += got

    for name in ("mw", "sc", "pg"):
        loads[name].wait()
    blockdiag[...] = jnp.zeros((chans, chans), BF16)
    for g in range(groups):
        lo = g * GROUP_DIM
        blockdiag[lo : lo + GROUP_DIM, lo : lo + GROUP_DIM] = mix_w[g]

    def share_squares(k, total):
        line = jnp.transpose(jnp.broadcast_to(total, (block, 128)))[:8]
        ss_buf[k, m] = line
        for j in range(1, tp):
            ss_copy(k, j, m).start()

    def row_factor(k, count):
        for j in range(1, tp):
            ss_copy(k, j, peer(j)).wait_recv()
        total = ss_buf[k, 0]
        for j in range(1, tp):
            total = total + ss_buf[k, j]
        line = lax.rsqrt(total[:1] * (1.0 / count) + EPS)
        return jnp.transpose(jnp.broadcast_to(line, (128, block)))[:, :1]

    position = s * block + lax.broadcasted_iota(jnp.int32, (block, 1), 0)
    since = position.astype(F32) + 1.0
    square_total = jnp.zeros((block, 1), F32)
    pw = 128
    means = []
    for c0 in range(0, chans, pw):
        current = ext[:, c0 : c0 + pw]
        channel = c0 + lax.broadcasted_iota(jnp.int32, (1, pw), 1)
        group = m * groups + channel // GROUP_DIM
        kind = lax.rem(group, 4)
        total = current
        chosen = jnp.zeros((block, pw), F32)
        for level in range(4):
            total = total + pltpu.roll(total, 1 << level, 0)
            share = 1.0 / jnp.minimum(since, float(2 << level))
            chosen = jnp.where(kind == level, total[RIM:] * share, chosen)
        means.append((chosen - current[RIM:]).astype(BF16))
    pooled = dot(jnp.concatenate(means, axis=1) if len(means) > 1 else means[0], blockdiag[...])
    pooled = pooled * scale[...]
    pooled_ref[...] = pooled
    share_squares(0, jnp.sum(pooled * pooled, axis=1, keepdims=True))

    @pl.when(s > 0)
    def _():
        arrive(1)

    for j in range(1, tp):
        for c in f_copy(s, j, peer(j)):
            c.wait_recv()
    expand(s)
    for h in range(heads):
        attend(h, True)

    @pl.when(s > 1)
    def _():
        arrive(2)

    pool_factor = row_factor(0, GROUPS * GROUP_DIM)
    mixed[...] = (pooled_ref[...] * pool_factor * pool_gain[...]).astype(BF16)
    loads["po"].wait()
    pool_mixed = mixed[...]

    def pool_chunk(c, carry):
        at = pl.multiple_of(c * cw, 128)
        acc_pool[:, pl.ds(at, cw)] = dot(pool_mixed, pool_out[:, pl.ds(at, cw)])
        return carry

    lax.fori_loop(0, chunks, pool_chunk, 0)

    def earlier(d, carry):
        src = s - d
        for j in range(1, tp):
            for c in f_copy(src, j, peer(j)):
                c.wait_recv()
        expand(src)
        for h in range(heads):
            attend(h, False)

        @pl.when(jnp.logical_and(d > 1, d < s))
        def _():
            arrive(d + 1)

        return carry

    lax.fori_loop(1, s + 1, earlier, 0)

    loads["ag"].wait()
    square_total = jnp.zeros((block, 1), F32)
    for h in range(heads):
        lo = h * VALUE_DIM
        one = acc[h, :, :VALUE_DIM] / acc[h, :, VALUE_DIM:]
        square_total = square_total + jnp.sum(one * one, axis=1, keepdims=True)
        mixed[:, lo : lo + VALUE_DIM] = (one * att_gain[:, lo : lo + VALUE_DIM]).astype(BF16)
    share_squares(1, square_total)
    loads["ao"].wait()
    factor_att = row_factor(1, HEADS * VALUE_DIM)
    att_mixed = mixed[...]
    for c in range(chunks):
        lo = c * cw
        part = dot(att_mixed, att_out[:, lo : lo + cw]) * factor_att + acc_pool[:, lo : lo + cw]
        send_buf[c] = part.astype(BF16).reshape(tp, rows, cw)
        for j in range(1, tp):
            out_copy(c, j, m).start()
    for c in range(chunks):
        total = send_buf[c, m].astype(F32)
        for j in range(1, tp):
            out_copy(c, j, peer(j)).wait_recv()
            total = total + recv_buf[c, peer(j)].astype(F32)
        out_ref[:, c * cw : (c + 1) * cw] = total.astype(BF16)

    for j in range(1, tp):
        tok_copy(j, m).wait_send()
        for k in range(2):
            ss_copy(k, j, m).wait_send()
        for c in range(chunks):
            out_copy(c, j, m).wait_send()
    for hop, wanted in hops:
        @pl.when(wanted)
        def _():
            for c in z_copy(hop, s):
                c.wait_send()

    def drain_relay(d, carry):
        @pl.when(relays(d))
        def _():
            for c in z_copy(0, s - d):
                c.wait_send()

        return carry

    lax.fori_loop(1, s + 1, drain_relay, 0)

    @pl.when(jnp.logical_and(s + 1 < sp, m == tp - 1))
    def _():
        for j in range(tp):
            tail_copy(j).wait_send()

    def drain(src, carry):
        for j in range(1, tp):
            for c in f_copy(src, j, m):
                c.wait_send()
        return carry

    lax.fori_loop(0, s + 1, drain, 0)


def turn_tables(length):
    steps = np.arange(HALF, dtype=np.float32) / np.float32(HALF)
    inv_freq = np.float32(1.0) / np.power(np.float32(THETA), steps).astype(np.float32)
    angle = inv_freq[:, None] * np.arange(length, dtype=np.float32)[None, :]
    angle = angle.astype(np.float32).astype(np.float64)
    return np.cos(angle).astype(np.float32), np.sin(angle).astype(np.float32)


def local(
    tokens, input_gain, query_weight, latent_down, rotary_down, pool_down, key_up, value_up,
    query_gain, key_gain, pool_weight, pool_scale, attention_gain, pool_gain, attention_out, pool_out,
):
    sp = lax.axis_size("sp")
    tp = lax.axis_size("tp")
    _, rows, width = tokens.shape
    block = rows * tp
    heads = HEADS // tp
    groups = GROUPS // tp
    chans = groups * GROUP_DIM
    cosine, sine = turn_tables(block * sp)
    chunks = 4
    cw = width // chunks
    line = lambda v: v.reshape(1, -1)
    operands = [
        tokens[0], line(input_gain), query_weight, latent_down, rotary_down.T, pool_down, key_up, value_up,
        line(query_gain), line(key_gain), pool_weight, line(pool_scale), line(attention_gain),
        line(pool_gain), attention_out, pool_out, jnp.asarray(cosine), jnp.asarray(sine),
    ]
    V = pltpu.VMEM
    D = pltpu.SemaphoreType.DMA
    held = [V(o.shape, o.dtype) for o in operands]
    held[0] = V((tp, rows, width), BF16)
    held[7] = V((KV_LATENT, heads * VALUE_DIM), BF16)
    held[10] = V((groups, GROUP_DIM, GROUP_DIM), BF16)
    scratch = held + [
        V((block + RIM, width), BF16),
        V((HEADS * NOPE_DIM, KV_LATENT), BF16),
        V((sp, tp, rows, KV_LATENT), BF16),
        V((sp, tp, ROPE_DIM, rows), BF16),
        V((heads, block, 128), BF16),
        V((heads, 128, block), BF16),
        V((heads, block, 2 * VALUE_DIM), BF16),
        V((heads, block, 2 * VALUE_DIM), F32),
        V((block + RIM, chans), F32),
        V((RIM, width), BF16),
        V((chans, chans), BF16),
        V((block, chans), F32),
        V((block, width), F32),
        V((2, tp, 8, block), F32),
        V((block, chans), BF16),
        V((chunks, tp, rows, cw), BF16),
        V((chunks, tp, rows, cw), BF16),
        D((len(operands),)),
        D((tp,)), D((tp,)),
        D((sp, 2, 2)), D((sp, 2)),
        D((sp, tp, 2)), D((sp, tp, 2)),
        D((tp,)), D((1,)),
        D((2, tp)), D((2, tp)),
        D((chunks, tp)), D((chunks, tp)),
    ]
    out = pl.pallas_call(
        functools.partial(kernel, sp, tp),
        out_shape=pltpu.VMEM((rows, width), BF16),
        in_specs=[pl.BlockSpec(memory_space=pltpu.HBM)] * len(operands),
        out_specs=pl.BlockSpec(memory_space=pltpu.VMEM),
        scratch_shapes=scratch,
        compiler_params=pltpu.CompilerParams(
            collective_id=0, has_side_effects=True, vmem_limit_bytes=56 * 1024 * 1024
        ),
    )(*operands)
    return out[None]


def solution(mesh):
    placed = (
        P("fs", ("sp", "tp"), None), P(), P(None, "tp"), P(), P(), P(None, "tp"), P(), P(),
        P(), P(), P(), P("tp"), P("tp"), P("tp"), P("tp", None), P("tp", None),
    )
    return jax.shard_map(
        local, mesh=mesh, in_specs=placed, out_specs=P("fs", ("sp", "tp"), None), check_vma=False
    )
```

```python
import functools
import math

import jax
import jax.numpy as jnp
import numpy as np
from jax import lax
from jax.experimental import pallas as pl
from jax.experimental.pallas import tpu as pltpu
from jax.sharding import PartitionSpec as P

HEADS = 8
NOPE_DIM = 64
ROPE_DIM = 32
VALUE_DIM = 128
KV_LATENT = 256
GROUPS = 16
GROUP_DIM = 64
QK_DIM = 96
EPS = 1e-06
THETA = 10000.0
RIM = 16
HALF = ROPE_DIM // 2
MESH = pl.DeviceIdType.MESH
F32 = jnp.float32
BF16 = jnp.bfloat16


def dot(a, b):
    return jnp.dot(a, b, preferred_element_type=F32)


def column_of(row, width):
    return jnp.transpose(jnp.broadcast_to(row, (128, width)))[:, :1]


def kernel(
    sp, tp,
    tokens_h, input_gain_h, query_w_h, latent_w_h, rotary_w_h, pool_w_h, key_up_h, value_up_h,
    query_gain_h, key_gain_h, mix_w_h, scale_h, att_gain_h, pool_gain_h, att_out_h, pool_out_h,
    cos_h, sin_h,
    out_ref,
    x_all, input_gain, query_w, latent_w, rotary_w, pool_w, key_up, value_up,
    query_gain, key_gain, mix_w, scale, att_gain, pool_gain, att_out, pool_out, cos_t, sin_t,
    normed, key_up_t, lat_buf, rot_buf, queries, keys_t, vals, acc, ext, tail_in, blockdiag,
    pooled_ref, acc_pool, ss_buf, mixed, send_buf, recv_buf,
    load_sem, tok_send, tok_recv, z_send, z_recv, f_send, f_recv, tail_send, tail_recv,
    ss_send, ss_recv, out_send, out_recv,
):
    s = lax.axis_index("sp")
    m = lax.axis_index("tp")
    rows, width = tokens_h.shape
    block = rows * tp
    heads = HEADS // tp
    groups = GROUPS // tp
    chans = groups * GROUP_DIM
    chunks, _, _, cw = send_buf.shape

    def peer(j):
        return lax.rem(m + j, tp)

    def load(i, src, dst):
        return pltpu.make_async_copy(src, dst, load_sem.at[i])

    loads = {
        "x": load(0, tokens_h, x_all.at[m]),
        "ig": load(1, input_gain_h, input_gain),
        "lw": load(2, latent_w_h, latent_w),
        "rw": load(3, rotary_w_h, rotary_w),
        "pw": load(4, pool_w_h, pool_w),
        "qw": load(5, query_w_h, query_w),
        "qg": load(6, query_gain_h, query_gain),
        "kg": load(7, key_gain_h, key_gain),
        "cos": load(8, cos_h, cos_t),
        "sin": load(9, sin_h, sin_t),
        "ku": load(10, key_up_h, key_up),
        "vu": load(11, value_up_h.at[:, pl.ds(pl.multiple_of(m * heads * VALUE_DIM, 128), heads * VALUE_DIM)], value_up),
        "mw": load(12, mix_w_h.at[pl.ds(m * groups, groups)], mix_w),
        "sc": load(13, scale_h, scale),
        "pg": load(14, pool_gain_h, pool_gain),
        "po": load(15, pool_out_h, pool_out),
        "ag": load(16, att_gain_h, att_gain),
        "ao": load(17, att_out_h, att_out),
    }
    first_loads = ("x", "ig", "lw", "rw", "qw", "qg", "cos", "sin", "pw")
    for name in first_loads:
        loads[name].start()

    barrier = pltpu.get_barrier_semaphore()
    for j in range(1, tp):
        pl.semaphore_signal(barrier, inc=1, device_id={"tp": peer(j)}, device_id_type=MESH)
    for d in range(1, sp):
        @pl.when(s >= d)
        def _():
            pl.semaphore_signal(barrier, inc=1, device_id={"sp": lax.rem(s + sp - d, sp)}, device_id_type=MESH)

    @pl.when(jnp.logical_and(s > 0, m < tp - 1))
    def _():
        where = {"sp": lax.rem(s + sp - 1, sp), "tp": tp - 1}
        pl.semaphore_signal(barrier, inc=1, device_id=where, device_id_type=MESH)

    def remote(src, dst, ssem, rsem, where):
        return pltpu.make_async_remote_copy(
            src_ref=src, dst_ref=dst, send_sem=ssem, recv_sem=rsem, device_id=where, device_id_type=MESH
        )

    def tok_copy(j, owner):
        return remote(tokens_h, x_all.at[owner], tok_send.at[j], tok_recv.at[owner], {"tp": peer(j)})

    def z_copy(hop, src):
        where = {"sp": lax.rem(s + hop + 1, sp)}
        return [
            remote(buf.at[src, m], buf.at[src, m], z_send.at[src, hop, k], z_recv.at[src, k], where)
            for k, buf in enumerate((lat_buf, rot_buf))
        ]

    odd = lax.rem(s, 2)
    hops = ((0, s + 1 < sp), (1, jnp.logical_and(s + 2 < sp, odd == 0)))

    def relays(d):
        return jnp.logical_and(s + 1 < sp, jnp.logical_or(odd == 0, d > 1))

    def arrive(d):
        src = s - d
        for c in z_copy(0, src):
            c.wait_recv()

        @pl.when(relays(d))
        def _():
            for c in z_copy(0, src):
                c.start()

        for j in range(1, tp):
            for c in f_copy(src, j, m):
                c.start()

    def f_copy(src, j, owner):
        where = {"tp": peer(j)}
        return [
            remote(buf.at[src, owner], buf.at[src, owner], f_send.at[src, j, k], f_recv.at[src, owner, k], where)
            for k, buf in enumerate((lat_buf, rot_buf))
        ]

    def tail_copy(j):
        where = {"sp": lax.rem(s + 1, sp), "tp": j}
        return remote(tokens_h.at[rows - RIM :, :], tail_in, tail_send.at[j], tail_recv.at[0], where)

    def ss_copy(k, j, owner):
        return remote(ss_buf.at[k, owner], ss_buf.at[k, owner], ss_send.at[k, j], ss_recv.at[k, owner], {"tp": peer(j)})

    def out_copy(c, j, owner):
        return remote(send_buf.at[c, peer(j)], recv_buf.at[c, owner], out_send.at[c, j], out_recv.at[c, owner], {"tp": peer(j)})

    apart = rows % 128 == 0
    step = min(64, rows)

    def slot_of(piece):
        return lax.rem(piece - m + tp, tp) if apart else piece

    def norm_rows(x):
        x = x.astype(F32)
        r = lax.rsqrt(jnp.mean(x * x, axis=-1, keepdims=True) + EPS)
        return (x * r * input_gain[...]).astype(BF16)

    def norm_piece(piece):
        first = slot_of(piece) * rows

        def body(i, carry):
            at = pl.multiple_of(i * step, step)
            to = pl.multiple_of(first + i * step, step)
            normed[pl.ds(to, step), :] = norm_rows(x_all[piece, pl.ds(at, step), :])
            return carry

        lax.fori_loop(0, rows // step, body, 0)

    loads["x"].wait()
    loads["ig"].wait()
    norm_piece(m)

    later = sp - 1 - s
    sends_tail = lax.div(m + 1, tp) * lax.div(later + max(sp - 2, 0), max(sp - 1, 1))
    pl.semaphore_wait(barrier, tp - 1 + later + sends_tail * (tp - 1))

    for j in range(1, tp):
        tok_copy(j, m).start()

    @pl.when(jnp.logical_and(s + 1 < sp, m == tp - 1))
    def _():
        for j in range(tp):
            tail_copy(j).start()

    loads["lw"].wait()
    loads["rw"].wait()
    own = normed[pl.ds(pl.multiple_of(slot_of(m) * rows, rows), rows), :]
    rot_buf[s, m] = lax.dot_general(
        rotary_w[...], own, (((1,), (1,)), ((), ())), preferred_element_type=F32
    ).astype(BF16)
    lat_buf[s, m] = dot(own, latent_w[...]).astype(BF16)
    for hop, wanted in hops:
        @pl.when(wanted)
        def _():
            for c in z_copy(hop, s):
                c.start()
    for j in range(1, tp):
        for c in f_copy(s, j, m):
            c.start()

    for name, item in loads.items():
        if name not in first_loads:
            item.start()

    loads["qw"].wait()
    loads["qg"].wait()
    loads["cos"].wait()
    loads["sin"].wait()
    factor = math.log2(math.e) / math.sqrt(QK_DIM)
    gain_q = column_of(query_gain[...], QK_DIM) * factor

    def project(slot, at, count, last):
        offset = slot * rows
        query_t = jnp.transpose(dot(normed[offset : offset + count, :], query_w[...]))
        first = pl.multiple_of(s * block + at, 128)
        cosine = cos_t[:, pl.ds(first, count)]
        sine = sin_t[:, pl.ds(first, count)]
        pad = jnp.zeros((128 - QK_DIM, count), F32)
        for h in range(heads):
            u = query_t[h * QK_DIM : (h + 1) * QK_DIM]
            r = lax.rsqrt(jnp.sum(u * u, axis=0, keepdims=True) * (1.0 / QK_DIM) + EPS)
            n = u * r * gain_q
            a = n[NOPE_DIM : NOPE_DIM + HALF]
            b = n[NOPE_DIM + HALF :]
            turned = jnp.concatenate(
                [n[:NOPE_DIM], a * cosine - b * sine, b * cosine + a * sine, pad], axis=0
            )
            queries[h, pl.ds(at, count), :] = jnp.transpose(turned).astype(BF16)
        taken = count
        if last:
            @pl.when(s > 0)
            def _():
                tail_copy(0).wait_recv()
                normed[block:, :] = norm_rows(tail_in[...])

            @pl.when(s == 0)
            def _():
                normed[block:, :] = jnp.zeros((RIM, width), BF16)

            taken = count + RIM
        pool_in = dot(normed[offset : offset + taken, :], pool_w[...]).astype(BF16).astype(F32)
        ext[pl.ds(pl.multiple_of(RIM + at, RIM), count), :] = pool_in[:count]
        if last:
            ext[:RIM, :] = pool_in[count:]

    loads["pw"].wait()
    if apart:
        for j in range(tp):
            if j > 0:
                tok_copy(j, peer(j)).wait_recv()
                norm_piece(peer(j))
            project(j, pl.multiple_of(peer(j) * rows, rows), rows, j == tp - 1)
    else:
        for j in range(1, tp):
            tok_copy(j, peer(j)).wait_recv()
            norm_piece(peer(j))
        project(0, 0, block, True)

    loads["ku"].wait()
    key_up_t[...] = jnp.transpose(key_up[...].astype(F32)).astype(BF16)
    loads["kg"].wait()
    gain_k = column_of(key_gain[...], QK_DIM)
    gain_k_plain = gain_k[:NOPE_DIM]
    gain_k_rot = gain_k[NOPE_DIM:]
    loads["vu"].wait()
    for h in range(heads):
        keys_t[h, QK_DIM:, :] = jnp.zeros((128 - QK_DIM, block), BF16)
        vals[h, :, VALUE_DIM:] = jnp.ones((block, VALUE_DIM), BF16)

    def expand(src):
        latent = lat_buf[src].reshape(block, KV_LATENT).astype(F32)
        r = lax.rsqrt(jnp.mean(latent * latent, axis=-1, keepdims=True) + EPS)
        latent_normed = (latent * r).astype(BF16)
        own_up = key_up_t[pl.ds(pl.multiple_of(m * heads * NOPE_DIM, 64), heads * NOPE_DIM), :]
        plain = lax.dot_general(
            own_up, latent_normed, (((1,), (1,)), ((), ())), preferred_element_type=F32
        )
        value = dot(latent_normed, value_up[...]).astype(BF16)
        pieces = [rot_buf[src, j].astype(F32) for j in range(tp)]
        shared = jnp.concatenate(pieces, axis=1) if tp > 1 else pieces[0]
        shared_sum = jnp.sum(shared * shared, axis=0, keepdims=True)
        first = pl.multiple_of(src * block, 128)
        cosine = cos_t[:, pl.ds(first, block)]
        sine = sin_t[:, pl.ds(first, block)]
        scaled = shared * gain_k_rot
        a = scaled[:HALF]
        b = scaled[HALF:]
        turned_a = a * cosine - b * sine
        turned_b = b * cosine + a * sine
        for h in range(heads):
            u = plain[h * NOPE_DIM : (h + 1) * NOPE_DIM]
            total = jnp.sum(u * u, axis=0, keepdims=True) + shared_sum
            r = lax.rsqrt(total * (1.0 / QK_DIM) + EPS)
            keys_t[h, :NOPE_DIM, :] = (u * gain_k_plain * r).astype(BF16)
            keys_t[h, NOPE_DIM : NOPE_DIM + HALF, :] = (turned_a * r).astype(BF16)
            keys_t[h, NOPE_DIM + HALF : QK_DIM, :] = (turned_b * r).astype(BF16)
            vals[h, :, :VALUE_DIM] = value[:, h * VALUE_DIM : (h + 1) * VALUE_DIM]

    qc = min(256, block)

    def attend(head, diagonal):
        for q0 in range(0, block, qc):
            span = q0 + qc if diagonal else block
            score = dot(queries[head, q0 : q0 + qc, :], keys_t[head, :, :span])
            weight = jnp.exp2(score)
            if diagonal:
                qpos = q0 + lax.broadcasted_iota(jnp.int32, (qc, span), 0)
                kpos = lax.broadcasted_iota(jnp.int32, (qc, span), 1)
                weight = jnp.where(kpos <= qpos, weight, 0.0)
            got = dot(weight.astype(BF16), vals[head, :span, :])
            if diagonal:
                acc[head, q0 : q0 + qc, :] = got
            else:
                acc[head, q0 : q0 + qc, :] += got

    for name in ("mw", "sc", "pg"):
        loads[name].wait()
    blockdiag[...] = jnp.zeros((chans, chans), BF16)
    for g in range(groups):
        lo = g * GROUP_DIM
        blockdiag[lo : lo + GROUP_DIM, lo : lo + GROUP_DIM] = mix_w[g]

    def share_squares(k, total):
        line = jnp.transpose(jnp.broadcast_to(total, (block, 128)))[:8]
        ss_buf[k, m] = line
        for j in range(1, tp):
            ss_copy(k, j, m).start()

    def row_factor(k, count):
        for j in range(1, tp):
            ss_copy(k, j, peer(j)).wait_recv()
        total = ss_buf[k, 0]
        for j in range(1, tp):
            total = total + ss_buf[k, j]
        line = lax.rsqrt(total[:1] * (1.0 / count) + EPS)
        return jnp.transpose(jnp.broadcast_to(line, (128, block)))[:, :1]

    position = s * block + lax.broadcasted_iota(jnp.int32, (block, 1), 0)
    since = position.astype(F32) + 1.0
    square_total = jnp.zeros((block, 1), F32)
    pw = 128
    means = []
    for c0 in range(0, chans, pw):
        current = ext[:, c0 : c0 + pw]
        channel = c0 + lax.broadcasted_iota(jnp.int32, (1, pw), 1)
        group = m * groups + channel // GROUP_DIM
        kind = lax.rem(group, 4)
        total = current
        chosen = jnp.zeros((block, pw), F32)
        for level in range(4):
            total = total + pltpu.roll(total, 1 << level, 0)
            share = 1.0 / jnp.minimum(since, float(2 << level))
            chosen = jnp.where(kind == level, total[RIM:] * share, chosen)
        means.append((chosen - current[RIM:]).astype(BF16))
    pooled = dot(jnp.concatenate(means, axis=1) if len(means) > 1 else means[0], blockdiag[...])
    pooled = pooled * scale[...]
    pooled_ref[...] = pooled
    share_squares(0, jnp.sum(pooled * pooled, axis=1, keepdims=True))

    @pl.when(s > 0)
    def _():
        arrive(1)

    for j in range(1, tp):
        for c in f_copy(s, j, peer(j)):
            c.wait_recv()
    expand(s)
    for h in range(heads):
        attend(h, True)

    @pl.when(s > 1)
    def _():
        arrive(2)

    pool_factor = row_factor(0, GROUPS * GROUP_DIM)
    mixed[...] = (pooled_ref[...] * pool_factor * pool_gain[...]).astype(BF16)
    loads["po"].wait()
    pool_mixed = mixed[...]

    def pool_chunk(c, carry):
        at = pl.multiple_of(c * cw, 128)
        acc_pool[:, pl.ds(at, cw)] = dot(pool_mixed, pool_out[:, pl.ds(at, cw)])
        return carry

    lax.fori_loop(0, chunks, pool_chunk, 0)

    def earlier(d, carry):
        src = s - d
        for j in range(1, tp):
            for c in f_copy(src, j, peer(j)):
                c.wait_recv()
        expand(src)
        for h in range(heads):
            attend(h, False)

        @pl.when(jnp.logical_and(d > 1, d < s))
        def _():
            arrive(d + 1)

        return carry

    lax.fori_loop(1, s + 1, earlier, 0)

    loads["ag"].wait()
    square_total = jnp.zeros((block, 1), F32)
    for h in range(heads):
        lo = h * VALUE_DIM
        one = acc[h, :, :VALUE_DIM] / acc[h, :, VALUE_DIM:]
        square_total = square_total + jnp.sum(one * one, axis=1, keepdims=True)
        mixed[:, lo : lo + VALUE_DIM] = (one * att_gain[:, lo : lo + VALUE_DIM]).astype(BF16)
    share_squares(1, square_total)
    loads["ao"].wait()
    factor_att = row_factor(1, HEADS * VALUE_DIM)
    att_mixed = mixed[...]
    for c in range(chunks):
        lo = c * cw
        part = dot(att_mixed, att_out[:, lo : lo + cw]) * factor_att + acc_pool[:, lo : lo + cw]
        send_buf[c] = part.astype(BF16).reshape(tp, rows, cw)
        for j in range(1, tp):
            out_copy(c, j, m).start()
    for c in range(chunks):
        total = send_buf[c, m].astype(F32)
        for j in range(1, tp):
            out_copy(c, j, peer(j)).wait_recv()
            total = total + recv_buf[c, peer(j)].astype(F32)
        out_ref[:, c * cw : (c + 1) * cw] = total.astype(BF16)

    for j in range(1, tp):
        tok_copy(j, m).wait_send()
        for k in range(2):
            ss_copy(k, j, m).wait_send()
        for c in range(chunks):
            out_copy(c, j, m).wait_send()
    for hop, wanted in hops:
        @pl.when(wanted)
        def _():
            for c in z_copy(hop, s):
                c.wait_send()

    def drain_relay(d, carry):
        @pl.when(relays(d))
        def _():
            for c in z_copy(0, s - d):
                c.wait_send()

        return carry

    lax.fori_loop(1, s + 1, drain_relay, 0)

    @pl.when(jnp.logical_and(s + 1 < sp, m == tp - 1))
    def _():
        for j in range(tp):
            tail_copy(j).wait_send()

    def drain(src, carry):
        for j in range(1, tp):
            for c in f_copy(src, j, m):
                c.wait_send()
        return carry

    lax.fori_loop(0, s + 1, drain, 0)


def turn_tables(length):
    steps = np.arange(HALF, dtype=np.float32) / np.float32(HALF)
    inv_freq = np.float32(1.0) / np.power(np.float32(THETA), steps).astype(np.float32)
    angle = inv_freq[:, None] * np.arange(length, dtype=np.float32)[None, :]
    angle = angle.astype(np.float32).astype(np.float64)
    return np.cos(angle).astype(np.float32), np.sin(angle).astype(np.float32)


def local(
    tokens, input_gain, query_weight, latent_down, rotary_down, pool_down, key_up, value_up,
    query_gain, key_gain, pool_weight, pool_scale, attention_gain, pool_gain, attention_out, pool_out,
):
    sp = lax.axis_size("sp")
    tp = lax.axis_size("tp")
    _, rows, width = tokens.shape
    block = rows * tp
    heads = HEADS // tp
    groups = GROUPS // tp
    chans = groups * GROUP_DIM
    cosine, sine = turn_tables(block * sp)
    chunks = 4
    cw = width // chunks
    line = lambda v: v.reshape(1, -1)
    operands = [
        tokens[0], line(input_gain), query_weight, latent_down, rotary_down.T, pool_down, key_up, value_up,
        line(query_gain), line(key_gain), pool_weight, line(pool_scale), line(attention_gain),
        line(pool_gain), attention_out, pool_out, jnp.asarray(cosine), jnp.asarray(sine),
    ]
    V = pltpu.VMEM
    D = pltpu.SemaphoreType.DMA
    held = [V(o.shape, o.dtype) for o in operands]
    held[0] = V((tp, rows, width), BF16)
    held[7] = V((KV_LATENT, heads * VALUE_DIM), BF16)
    held[10] = V((groups, GROUP_DIM, GROUP_DIM), BF16)
    scratch = held + [
        V((block + RIM, width), BF16),
        V((HEADS * NOPE_DIM, KV_LATENT), BF16),
        V((sp, tp, rows, KV_LATENT), BF16),
        V((sp, tp, ROPE_DIM, rows), BF16),
        V((heads, block, 128), BF16),
        V((heads, 128, block), BF16),
        V((heads, block, 2 * VALUE_DIM), BF16),
        V((heads, block, 2 * VALUE_DIM), F32),
        V((block + RIM, chans), F32),
        V((RIM, width), BF16),
        V((chans, chans), BF16),
        V((block, chans), F32),
        V((block, width), F32),
        V((2, tp, 8, block), F32),
        V((block, chans), BF16),
        V((chunks, tp, rows, cw), BF16),
        V((chunks, tp, rows, cw), BF16),
        D((len(operands),)),
        D((tp,)), D((tp,)),
        D((sp, 2, 2)), D((sp, 2)),
        D((sp, tp, 2)), D((sp, tp, 2)),
        D((tp,)), D((1,)),
        D((2, tp)), D((2, tp)),
        D((chunks, tp)), D((chunks, tp)),
    ]
    out = pl.pallas_call(
        functools.partial(kernel, sp, tp),
        out_shape=pltpu.VMEM((rows, width), BF16),
        in_specs=[pl.BlockSpec(memory_space=pltpu.HBM)] * len(operands),
        out_specs=pl.BlockSpec(memory_space=pltpu.VMEM),
        scratch_shapes=scratch,
        compiler_params=pltpu.CompilerParams(
            collective_id=0, has_side_effects=True, vmem_limit_bytes=56 * 1024 * 1024
        ),
    )(*operands)
    return out[None]


def solution(mesh):
    placed = (
        P("fs", ("sp", "tp"), None), P(), P(None, "tp"), P(), P(), P(None, "tp"), P(), P(),
        P(), P(), P(), P("tp"), P("tp"), P("tp"), P("tp", None), P("tp", None),
    )
    return jax.shard_map(
        local, mesh=mesh, in_specs=placed, out_specs=P("fs", ("sp", "tp"), None), check_vma=False
    )
```
